32 devices in a mesh: ep: 8 (over z, core), tp: 4 (over y, x).
Axes of the slice: x: 2, y: 2, z: 4, core: 2. Of those that a mesh axis runs over, the one named last changes fastest.
Arguments:
- tokens: bfloat16 [1024, 2048], P('ep', 'tp')
- norm_gain: float32 [2048], P('tp'), may hold values from 0.1 to 1.9
- routing: int32 [1024, 2], P('ep'), may hold values from 0 to 3, all different within a row; in each aligned block of 128 rows (0 to 127, 128 to 255, ...) at most 80 rows name the same one
- route_weight: float32 [1024, 2], P('ep'), may hold values from 0.1 to 1
- gate_weight: bfloat16 [8, 2048, 3584], P('ep', None, 'tp'), may hold values from -0.125 to 0.125
- up_weight: bfloat16 [8, 2048, 3584], P('ep', None, 'tp'), may hold values from -0.125 to 0.125
- down_weight: bfloat16 [8, 3584, 2048], P('ep', None, 'tp')
- final_gain: float32 [2048], P('tp'), may hold values from 0.1 to 1.9
Outputs:
- mixed: bfloat16 [1024, 2048], P('ep', 'tp')
The draws below stay inside these ranges and needn't reach their ends.
Inputs may be any that keep to these rules, and one draw needn't show every extreme that they name: `routing`: each row names 2 different experts. Among the 128 rows of one device along ep (aligned blocks), no expert is named more than 80 times, a bound that some blocks reach.
All inputs are finite; a program needn't handle non-finite values.
Results may differ from the reference program's by a relative error of at most 0.0077.
Values may be sent and summed in bfloat16 or wider, within the bound.
A program may use at most 64 MiB of HBM per device.

```python
import math
import jax
import jax.numpy as jnp
import numpy as np
from jax import lax

D = 2048
FF = 7168
TOPK = 2
TOK_DEV = 128
EXPERTS = 4
CAP = 80
TOKENS = 1024
N_EP = 8


def draw_tokens(key, part):
    column = jnp.arange(D, dtype=jnp.float32) / D
    values = jax.random.normal(key, (TOKENS, D), jnp.float32) * 10.0 ** (0.8 * column)
    return values.astype(jnp.bfloat16)


def draw_down_weight(key, part):
    column = jnp.arange(D, dtype=jnp.float32) / D
    scale = (FF // 2) ** (-0.5) * 10.0 ** (0.8 * column)
    values = jax.random.normal(key, (2 * EXPERTS, FF // 2, D), jnp.float32)
    return (values * scale).astype(jnp.bfloat16)


def block_scale(rng, dims, cuts, low, high):
    level, own = 1.0, jax.random.fold_in(rng, 6)
    for position, shards_of in cuts:
        steps = jnp.exp(jax.random.uniform(jax.random.fold_in(own, position), (shards_of,), jnp.float32, low / len(cuts), high / len(cuts)))
        level = level * jnp.repeat(steps, dims[position] // shards_of).reshape([-1 if axis == position else 1 for axis in range(len(dims))])
    return level


def shared_out(own_key, own, number, rows, count, top, most, lean):
    order = jax.random.permutation(own_key, count)
    crowded, usual = portions_of(count, rows * top, most, lean, True), portions_of(count, rows * top, most, lean, False)
    places = jnp.arange(count)

    def named(sizes, rotation):
        used = int((sizes > 0).sum())
        fixed = max(1, used // 4)
        passed = fixed + (places - fixed + rotation * (used - fixed)) % max(1, count - fixed)
        return jnp.zeros((count,), jnp.int32).at[order[jnp.where(places < fixed, places, passed)]].set(jnp.asarray(sizes, jnp.int32))

    sizes = jnp.where(number % 4 == 0, named(crowded, number // 4), named(usual, number - number // 4 - 1))
    mixed = jax.random.permutation(jax.random.fold_in(own, 3), count)
    source_of, receiver = mixed[0:count // 2 * 2:2], mixed[1:count // 2 * 2:2]
    room = jnp.minimum(sizes[source_of] - 1, most - sizes[receiver]) // 2
    room = jnp.where((source_of == order[0]) | (receiver == order[0]) | (sizes[receiver] == 0), 0, jnp.maximum(room, 0))
    passed = jax.random.randint(jax.random.fold_in(own, 4), (count // 2,), 0, 1 << 20) % (room + 1)
    sizes = sizes.at[source_of].add(-passed).at[receiver].add(passed)
    members = jnp.searchsorted(jnp.cumsum(sizes), jnp.arange(rows * top), side="right").astype(jnp.int32)
    grid = members.reshape(top, rows).T
    grid = grid[jax.random.permutation(jax.random.fold_in(own, 1), rows)]
    rotation = jax.random.randint(jax.random.fold_in(own, 2), (rows, 1), 0, top)
    return jnp.take_along_axis(grid, (jnp.arange(top)[None, :] + rotation) % top, axis=1)


def portions_of(amount, total, limit, lean, full):
    portions = [(1 << 20) // math.isqrt(standing ** lean) + 1 for standing in range(1, amount + 1)]
    largest = limit if full else min(limit, max(-(-total // amount), total * portions[0] // sum(portions)))
    least = 1 if total - largest >= amount - 1 else 0
    given, surplus = [largest] + [least] * (amount - 1), total - largest - least * (amount - 1)
    while surplus > 0:
        movable = [i for i in range(1, amount) if given[i] < largest] or [i for i in range(1, amount) if given[i] < limit]
        pool, budget = sum([portions[i] for i in movable]), surplus
        for i in movable:
            extra = min(limit - given[i], max(1, budget * portions[i] // pool), surplus)
            given[i] = given[i] + extra
            surplus = surplus - extra
    return np.array(given)


def scatter_about(key, extent, deviation, most, shards=(), held_as=jnp.bfloat16):
    array = jax.random.normal(key, extent, jnp.float32) * deviation
    if len(shards) > 0:
        array = block_scale(key, extent, shards, -0.22, 0.18) * array
    return jnp.clip(array, min=-most, max=most).astype(held_as)


def setup_inputs(seed: int = 0) -> dict:
    seeds = jax.random.split(jax.random.key(seed), 9)
    tokens = draw_tokens(jax.random.fold_in(seeds[8], 71), 0)
    norm_gain = jnp.clip(1.0 + 0.18 * jax.random.normal(seeds[1], (D,), jnp.float32), 0.1, 1.9)
    routing_keys = jax.random.split(jax.random.fold_in(seeds[2], 1), TOKENS // TOK_DEV)
    routing_turns = jax.random.permutation(jax.random.fold_in(seeds[2], 3), TOKENS // TOK_DEV)
    routing = jax.vmap(lambda own, number: shared_out(jax.random.fold_in(seeds[2], 2), own, number, TOK_DEV, EXPERTS, TOPK, CAP, 2))(routing_keys, routing_turns).reshape((TOKENS, TOPK))
    route_weight = jnp.clip(0.1 + 0.9 * jax.random.uniform(seeds[3], (TOKENS, TOPK), jnp.float32) ** block_scale(seeds[3], (TOKENS, TOPK), ((0, 8),), -0.2, 0.2), 0.1, 1.0)
    gate_weight = scatter_about(seeds[4], (2 * EXPERTS, D, FF // 2), D ** -0.5, 0.125, ((0, 8), (2, 4)))
    up_weight = scatter_about(seeds[5], (2 * EXPERTS, D, FF // 2), D ** -0.5, 0.125, ((0, 8), (2, 4)))
    down_weight = draw_down_weight(jax.random.fold_in(seeds[8], 71), 0)
    final_gain = jnp.clip(1.0 + 0.18 * jax.random.normal(seeds[7], (D,), jnp.float32), 0.1, 1.9)
    return dict(tokens=tokens, norm_gain=norm_gain, routing=routing, route_weight=route_weight, gate_weight=gate_weight, up_weight=up_weight, down_weight=down_weight, final_gain=final_gain)


EPS = 1e-05

def rms_scale(values, gain):
    return values * lax.rsqrt(lax.optimization_barrier(jnp.mean(values * values, axis=-1, keepdims=True)) + EPS) * gain

def slot_numbers(expert_ids):
    onehot = (expert_ids[..., None] == jnp.arange(EXPERTS, dtype=jnp.int32)).astype(jnp.int32)
    before = jnp.cumsum(onehot, axis=1) - onehot
    return lax.optimization_barrier(jnp.sum(before * onehot, axis=2)).astype(jnp.int32)

def reference(tokens, norm_gain, routing, route_weight, gate_weight, up_weight, down_weight, final_gain):
    normed = rms_scale(tokens.astype(jnp.float32), norm_gain).astype(jnp.bfloat16)
    copies = TOK_DEV * TOPK
    expert_ids = routing.reshape(N_EP, copies).astype(jnp.int32)
    slot_index = slot_numbers(expert_ids)
    source_index = jnp.broadcast_to(jnp.arange(N_EP, dtype=jnp.int32)[:, None], (N_EP, copies))
    token_index = jnp.broadcast_to((jnp.arange(copies, dtype=jnp.int32) // TOPK)[None, :], (N_EP, copies))
    source_rows = normed.reshape(N_EP, TOK_DEV, D)[source_index, token_index]

    def one_expert(expert):
        target = jnp.where(expert_ids == expert, slot_index, CAP)
        buffer = jnp.zeros((N_EP, CAP, D), jnp.bfloat16).at[source_index, target].set(source_rows, mode='drop')
        buffer = buffer.reshape(N_EP * CAP, D)
        results = []
        for half_index in range(2):
            row = 2 * expert + half_index
            gate_half = lax.dynamic_index_in_dim(gate_weight, row, 0, keepdims=False)
            up_half = lax.dynamic_index_in_dim(up_weight, row, 0, keepdims=False)
            down_half = lax.dynamic_index_in_dim(down_weight, row, 0, keepdims=False)
            gate = jnp.dot(buffer, gate_half, preferred_element_type=jnp.float32)
            upper = jnp.dot(buffer, up_half, preferred_element_type=jnp.float32)
            hidden = (jax.nn.silu(gate) * upper).astype(jnp.bfloat16)
            results.append(jnp.dot(hidden, down_half, preferred_element_type=jnp.float32).astype(jnp.bfloat16))
        return jnp.stack(results)
    results = lax.map(one_expert, jnp.arange(EXPERTS, dtype=jnp.int32))
    results = results.reshape(EXPERTS, 2, N_EP, CAP, D)
    picked = results[expert_ids, :, source_index, slot_index]
    paired = (picked[:, :, 0].astype(jnp.float32) + picked[:, :, 1].astype(jnp.float32)).astype(jnp.bfloat16)
    paired = lax.optimization_barrier(paired)
    summed = paired.astype(jnp.float32)
    weights = route_weight.reshape(N_EP, copies).astype(jnp.float32)
    mixed_sum = lax.optimization_barrier(jnp.sum((summed * weights[..., None]).reshape(N_EP, TOK_DEV, TOPK, D), axis=2))
    mixed_sum = mixed_sum.reshape(TOKENS, D)
    return rms_scale(mixed_sum, final_gain).astype(jnp.bfloat16)
```

```python
import contextlib
import functools

import jax
import jax.numpy as jnp
from jax import lax
from jax.experimental import pallas as pl
from jax.experimental.pallas import tpu as pltpu
from jax.sharding import PartitionSpec as P

TOPK = 2
EPS = 1e-05
MESH = pl.DeviceIdType.MESH
F32, BF16 = jnp.float32, jnp.bfloat16


def flipped(index, mask):
    out, bit = index, 1
    while bit <= mask:
        if mask & bit:
            out = out + bit - 2 * bit * ((index // bit) % 2)
        bit *= 2
    return out


def dot(a, b):
    return jnp.dot(a, b, preferred_element_type=F32)


def dot_t(a, b):
    return lax.dot_general(a, b, (((0,), (0,)), ((), ())), preferred_element_type=F32)


def scope(name):
    return contextlib.nullcontext()


def order(groups, per):
    late = list(range(2, groups)) + [g for g in (1, 0) if g < groups]
    steps = [("gains",), ("gs", 0), ("disp",), ("gr", 0)] if per == 1 else [
        ("gains",), ("disp",), ("gs", 0), ("gr", 0)
    ]
    if groups > 1:
        steps += [("gs", 1)]
    steps += [("gainw",)]
    for g in range(groups):
        steps += [("ge", g), ("up", g)]
        if g == 0 and groups > 1:
            steps += [("gr", 1)]
        if g + 2 < groups:
            steps += [("gs", g + 2)]
        if g and g + 1 < groups:
            steps += [("gr", g + 1)]
        if g == groups - 1 and g > 2:
            steps += [("hr", g - 1)]
        steps += [("hs", g)]
    steps += [("wd",)]
    relayed = [late[0]] if groups > 3 else []
    if relayed:
        steps += [("down", late[0])]
    steps += [("hr", g) for g in late if g not in relayed]
    steps += [("comb", g) for g in relayed]
    for g in late:
        if g not in relayed:
            steps += [("down", g), ("comb", g)]
    return steps


def sequence(groups, per):
    late = list(range(2, groups)) + [g for g in (1, 0) if g < groups]
    return [k for g in late for k in range(g * per, (g + 1) * per) if k] + [0]


def kernel(
    n, planes, groups,
    tokens_hbm, gain_hbm, routing_hbm, weight_hbm, gate_hbm, up_hbm, down_hbm, final_hbm,
    out,
    tokens, routing_t, weight_t, final_gain,
    wg, wu, wd, gains, picked, x, xn, hid, half_own, half_send, half_recv, pair, comb, sq_out, sq_in,
    in_sem, w_sem, gain_s, gain_r, disp_s, disp_r, x_s, x_r, d2d_s, d2d_r, h_s, h_r, po_s, po_r,
    c_s, c_r, sq_s, sq_r,
):
    ep, t = lax.axis_index("ep"), lax.axis_index("tp")
    z, core = ep // 2, ep % 2
    partner = (ep + 1 - 2 * core, t)
    pieces, cap, part = picked.shape[1:]
    width = pieces * part
    per = planes // groups
    rows = per * cap
    inner = hid.shape[-1]
    tok_rows = tokens.shape[0]
    depth = n * width
    bits = [1 << b for b in range(n.bit_length() - 1)]
    tp_peer = [(ep, flipped(t, j)) for j in range(n)]
    tp_index = [flipped(t, j) for j in range(n)]
    expert = [flipped(z, k) for k in range(planes)]
    plane_peer = [(2 * expert[k] + core, t) for k in range(planes)]

    barrier = pltpu.get_barrier_semaphore()
    peers = tp_peer[1:] + plane_peer[1:] + [partner]
    for peer in peers:
        pl.semaphore_signal(barrier, inc=1, device_id=peer, device_id_type=MESH)

    inputs = [
        pltpu.make_async_copy(src, dst, in_sem.at[i])
        for i, (src, dst) in enumerate((
            (tokens_hbm, tokens), (routing_hbm, routing_t), (gain_hbm, gains.at[0]),
            (weight_hbm, weight_t), (final_hbm, final_gain),
        ))
    ]
    loads = [
        pltpu.make_async_copy(src.at[0], dst, w_sem.at[i])
        for i, (src, dst) in enumerate(((gate_hbm, wg), (up_hbm, wu), (down_hbm, wd)))
    ]
    for load in inputs + loads:
        load.start()
    for load in inputs[:3]:
        load.wait()

    token_row = lax.broadcasted_iota(jnp.int32, (tok_rows, tok_rows), 0)
    token_col = lax.broadcasted_iota(jnp.int32, (tok_rows, tok_rows), 1)
    r_t0, r_t1 = routing_t[0:1, :], routing_t[1:2, :]
    wide = -(-planes // 16) * 16
    sub = lax.broadcasted_iota(jnp.int32, (wide, tok_rows), 0)
    member_t = jnp.zeros((wide, tok_rows), F32)
    for k in range(planes):
        named = ((r_t0 == expert[k]) | (r_t1 == expert[k])).astype(F32)
        member_t = jnp.where(sub == k, named, member_t)
    earlier = (token_row < token_col).astype(F32).astype(BF16)
    slot_t = dot(member_t.astype(BF16), earlier)
    slot_t = jnp.where(member_t > 0, slot_t, -1.0)
    slot_sub = lax.broadcasted_iota(jnp.int32, (cap, tok_rows), 0).astype(F32)

    def pick(k, to):
        chosen = (slot_sub == slot_t[k : k + 1, :]).astype(F32).astype(BF16)
        rows_of = dot(chosen, tokens[...]).astype(BF16)
        for half in range(pieces):
            to[half] = rows_of[:, half * part : (half + 1) * part]

    sent = []

    def remote(src, dst, s, r, peer):
        return pltpu.make_async_remote_copy(
            src_ref=src, dst_ref=dst, send_sem=s, recv_sem=r, device_id=peer, device_id_type=MESH
        )

    def start(copy):
        copy.start()
        sent.append(copy)
        return copy

    pick(0, x.at[0, 0, 0, :, 0])
    for k in range(1, planes):
        pick(k, picked.at[k])

    with scope("barrier"):
        pl.semaphore_wait(barrier, len(peers))

    disp = [
        None if k == 0 else remote(
            picked.at[k], x.at[k // per, 0, 0, :, k % per], disp_s.at[k], disp_r.at[k], plane_peer[k]
        )
        for k in range(planes)
    ]
    def tree(at, send_sem, recv_sem, order):
        copies, need = {}, {0: []}
        have = [0]
        for position, bit in enumerate(order):
            for j in list(have):
                into = j ^ bit
                copies[into] = remote(at(j), at(into), send_sem(into), recv_sem(into), tp_peer[bit])
                need[j].append(into)
                need[into] = []
                have.append(into)
        return copies, need, have[1:]

    def ascending(g):
        return bits if g % 2 == 0 else bits[::-1]

    trees = [
        [
            tree(
                lambda j, g=g, half=half: x.at[g, j, 0, half],
                lambda j, g=g, half=half: x_s.at[g, half, j],
                lambda j, g=g, half=half: x_r.at[g, half, j], ascending(half if pieces > 1 else g),
            )
            for half in range(pieces)
        ]
        for g in range(groups)
    ]
    across = [
        [
            [
                remote(
                    x.at[g, j, 0, half], x.at[g, j, 1, half],
                    d2d_s.at[g, half, j], d2d_r.at[g, half, j], partner,
                )
                for j in range(n)
            ]
            for half in range(pieces)
        ]
        for g in range(groups)
    ]
    hidden_trees = [
        [
            tree(
                lambda j, g=g, side=side: hid.at[g, j, side],
                lambda j, g=g, side=side: h_s.at[g, side, j],
                lambda j, g=g, side=side: h_r.at[g, side, j], ascending(side),
            )
            for side in range(2)
        ]
        for g in range(groups)
    ]

    def gather_start(g):
        for k in range(max(1, g * per), (g + 1) * per):
            disp[k].wait_recv()
        for step in range(len(bits)):
            for half in range(pieces):
                copies, need, _ = trees[g][half]
                start(copies[need[0][step]])
        for half in range(pieces):
            start(across[g][half][0])

    def gather_relay(g):
        for half in range(pieces):
            copies, need, arrivals = trees[g][half]
            for j in arrivals:
                if need[j]:
                    copies[j].wait_recv()
                    for into in need[j]:
                        start(copies[into])
                    start(across[g][half][j])

    def gather_end(g):
        for last in range(2):
            for half in range(pieces):
                copies, need, arrivals = trees[g][half]
                for j in arrivals:
                    if not need[j] and (j == n - 1) == bool(last):
                        copies[j].wait_recv()
                        start(across[g][half][j])
        for half in range(pieces):
            for j in range(n):
                across[g][half][j].wait_recv()

    def upward(g):
        blocks = [
            [x[g, j, :, half].reshape(2 * rows, part).astype(F32) for half in range(pieces)] for j in range(n)
        ]
        square = sum(jnp.sum(p * p, axis=1, keepdims=True) for of_peer in blocks for p in of_peer)
        scale = lax.rsqrt(square / depth + EPS)
        for j in range(n):
            for half in range(pieces):
                columns = pl.ds(pl.multiple_of(tp_index[j] * width + half * part, part), part)
                own = gains[j, :, half * part : (half + 1) * part]
                xn[:, columns] = (blocks[j][half] * scale * own).astype(BF16)
        for first in range(0, inner, 256):
            last = min(first + 256, inner)
            left = dot(xn[...], wg[:, first:last])
            right = dot(xn[...], wu[:, first:last])
            value = (jax.nn.silu(left) * right).astype(BF16)
            hid[g, 0, :, :, first:last] = value.reshape(2, rows, last - first)

    def hidden_start(g):
        for step in range(len(bits)):
            for side in range(2):
                copies, need, _ = hidden_trees[g][side]
                start(copies[need[0][step]])

    def hidden_relay(g):
        for side in range(2):
            copies, need, arrivals = hidden_trees[g][side]
            for j in arrivals:
                if need[j]:
                    copies[j].wait_recv()
                    for into in need[j]:
                        start(copies[into])

    halves = [
        remote(half_send.at[g], half_recv.at[g], po_s.at[g], po_r.at[g], partner) for g in range(groups)
    ]

    def downward(g):
        total = None
        for j in range(n):
            for side in range(2):
                copies, need, _ = hidden_trees[g][side]
                if j and not need[j]:
                    copies[j].wait_recv()
            part = wd[pl.ds(pl.multiple_of(tp_index[j] * inner, inner), inner), :]
            term = dot(hid[g, j].reshape(2 * rows, inner), part)
            total = term if total is None else total + term
        half_own[g] = total[:rows].astype(BF16)
        half_send[g] = total[rows:].astype(BF16)
        start(halves[g])

    back = [
        None if k == 0 else remote(
            pair.at[k // per, k % per], comb.at[k], c_s.at[k], c_r.at[k], plane_peer[k]
        )
        for k in range(planes)
    ]

    def combine(g):
        halves[g].wait_recv()
        both = (half_own[g].astype(F32) + half_recv[g].astype(F32)).astype(BF16)
        pair[g] = both.reshape(per, cap, width)
        for k in range(g * per, (g + 1) * per):
            if k == 0:
                comb[0] = both[:cap]
            else:
                start(back[k])

    gain_copies = [
        remote(gains.at[0], gains.at[j], gain_s.at[j], gain_r.at[j], tp_peer[j]) for j in range(1, n)
    ]

    def dispatch():
        for k in range(1, planes):
            start(disp[k])

    def gains_start():
        for copy in gain_copies:
            start(copy)

    def gains_end():
        for copy in gain_copies:
            copy.wait_recv()
        for load in inputs[3:]:
            load.wait()
        loads[0].wait()
        loads[1].wait()

    def run(steps):
        for name, *of in steps:
            with scope(name + "".join(str(g) for g in of)):
                actions[name](*of)

    actions = dict(
        disp=dispatch, gs=gather_start, gr=gather_relay, ge=gather_end, up=upward, hs=hidden_start,
        hr=hidden_relay, gains=gains_start, gainw=gains_end, wd=lambda: loads[2].wait(),
        down=downward, comb=combine,
    )
    run(order(groups, per))

    w_t0, w_t1 = weight_t[0:1, :], weight_t[1:2, :]

    def share(k):
        weight = jnp.where(r_t0 == expert[k], w_t0, w_t1)
        table = jnp.where(slot_sub == slot_t[k : k + 1, :], weight, 0.0)
        high = table.astype(BF16)
        rest = table - high.astype(F32)
        middle = rest.astype(BF16)
        low = (rest - middle.astype(F32)).astype(BF16)
        block = comb[k]
        return dot_t(high, block) + (dot_t(middle, block) + dot_t(low, block))

    mixed = None
    for k in sequence(groups, per):
        with scope(f"share{k}"):
            if k:
                back[k].wait_recv()
            mixed = share(k) if mixed is None else mixed + share(k)

    square = jnp.sum(mixed * mixed, axis=1, keepdims=True)
    sq_out[...] = jnp.transpose(jnp.broadcast_to(square, (tok_rows, 128)))[0:8, :]
    sums = [remote(sq_out, sq_in.at[j], sq_s.at[j], sq_r.at[j], tp_peer[j]) for j in range(1, n)]
    for copy in sums:
        start(copy)
    total = sq_out[...]
    with scope("sqwait"):
        for j in range(1, n):
            sums[j - 1].wait_recv()
            total = total + sq_in[j]
    column = jnp.transpose(jnp.broadcast_to(total[0:1, :], (128, tok_rows)))[:, 0:1]
    out[...] = (mixed * lax.rsqrt(column / depth + EPS) * final_gain[...]).astype(BF16)
    with scope("wsend"):
        for copy in sent:
            copy.wait_send()


def shards(
    tokens, norm_gain, routing, route_weight, gate_weight, up_weight, down_weight, final_gain
):
    ep_count, n = lax.axis_size("ep"), lax.axis_size("tp")
    planes = ep_count // 2
    tok_rows, width = tokens.shape
    capacity = 2 * ((tok_rows * TOPK * 5 + planes * 8 - 1) // (planes * 8))
    cap = -(-capacity // 16) * 16
    groups = min(4, planes)
    per = planes // groups
    rows = per * cap
    pieces = 2 if width % 256 == 0 else 1
    part = width // pieces
    depth, inner = gate_weight.shape[1:]
    dma = pltpu.SemaphoreType.DMA
    vmem, anywhere = pl.BlockSpec(memory_space=pltpu.VMEM), pl.BlockSpec(memory_space=pl.ANY)
    return pl.pallas_call(
        functools.partial(kernel, n, planes, groups),
        out_shape=pltpu.VMEM((tok_rows, width), BF16),
        in_specs=[anywhere] * 8,
        out_specs=vmem,
        scratch_shapes=[
            pltpu.VMEM((tok_rows, width), BF16),
            pltpu.VMEM((TOPK, tok_rows), jnp.int32),
            pltpu.VMEM((TOPK, tok_rows), F32),
            pltpu.VMEM((1, width), F32),
            pltpu.VMEM((depth, inner), BF16),
            pltpu.VMEM((depth, inner), BF16),
            pltpu.VMEM((n * inner, width), BF16),
            pltpu.VMEM((n, 1, width), F32),
            pltpu.VMEM((planes, pieces, cap, part), BF16),
            pltpu.VMEM((groups, n, 2, pieces, per, cap, part), BF16),
            pltpu.VMEM((2 * rows, depth), BF16),
            pltpu.VMEM((groups, n, 2, rows, inner), BF16),
            pltpu.VMEM((groups, rows, width), BF16),
            pltpu.VMEM((groups, rows, width), BF16),
            pltpu.VMEM((groups, rows, width), BF16),
            pltpu.VMEM((groups, per, cap, width), BF16),
            pltpu.VMEM((planes, cap, width), BF16),
            pltpu.VMEM((8, 128), F32),
            pltpu.VMEM((n, 8, 128), F32),
            dma((5,)), dma((3,)), dma((n,)), dma((n,)), dma((planes,)), dma((planes,)),
            dma((groups, pieces, n)), dma((groups, pieces, n)), dma((groups, pieces, n)), dma((groups, pieces, n)),
            dma((groups, 2, n)), dma((groups, 2, n)), dma((groups,)), dma((groups,)),
            dma((planes,)), dma((planes,)), dma((n,)), dma((n,)),
        ],
        compiler_params=pltpu.CompilerParams(
            collective_id=0, has_side_effects=True, vmem_limit_bytes=60 * 1024 * 1024
        ),
    )(
        tokens, norm_gain.reshape(1, width), routing.T, route_weight.T,
        gate_weight, up_weight, down_weight, final_gain.reshape(1, width),
    )


def solution(mesh):
    placed = (
        P("ep", "tp"),
        P("tp"),
        P("ep", None),
        P("ep", None),
        P("ep", None, "tp"),
        P("ep", None, "tp"),
        P("ep", None, "tp"),
        P("tp"),
    )
    return jax.shard_map(
        shards, mesh=mesh, in_specs=placed, out_specs=P("ep", "tp"), check_vma=False
    )
```

```python
import contextlib
import functools

import jax
import jax.numpy as jnp
from jax import lax
from jax.experimental import pallas as pl
from jax.experimental.pallas import tpu as pltpu
from jax.sharding import PartitionSpec as P

TOPK = 2
EPS = 1e-05
MESH = pl.DeviceIdType.MESH
F32, BF16 = jnp.float32, jnp.bfloat16


def scope(name):
    return contextlib.nullcontext()


def flipped(index, mask):
    out, bit = index, 1
    while bit <= mask:
        if mask & bit:
            out = out + bit - 2 * bit * ((index // bit) % 2)
        bit *= 2
    return out


def dot(a, b):
    return jnp.dot(a, b, preferred_element_type=F32)


def dot_t(a, b):
    return lax.dot_general(a, b, (((0,), (0,)), ((), ())), preferred_element_type=F32)


def spread(n, backwards):
    bits = [1 << b for b in range(n.bit_length() - 1)]
    edges, need, have = [], {0: []}, [0]
    for bit in bits[::-1] if backwards else bits:
        for j in list(have):
            edges.append((j, j ^ bit, bit))
            need[j].append(j ^ bit)
            need[j ^ bit] = []
            have.append(j ^ bit)
    return edges, need, have[1:]


def arrivals(n, ways):
    slots, count = {}, 0
    trees = [spread(n, backwards) for backwards in ways]
    for j in range(1, n):
        alone = any(need[j] for _, need, _ in trees)
        for i in range(len(ways)):
            slots[i, j] = count
            count += alone
        count += not alone
    return slots, count


def wide_groups(planes, per):
    return (1, 2) if per == 1 and planes == 4 else ()


def ways_of(pieces, g):
    return [bool(i % 2) for i in range(pieces)] if pieces > 1 else [bool(g % 2)]


def order(groups, per, wide):
    if wide:
        return [
            ("first",), ("trelay",), ("tend",), ("gs", 3), ("loaded",), ("xs", 0), ("up", 0), ("gr", 3), ("hs", 0),
            ("ge", 3), ("xs", 3), ("up", 3), ("hs", 3), ("xw", 1), ("xs", 1), ("up", 1), ("hs", 1), ("hr", 3),
            ("xw", 2), ("xs", 2), ("up", 2), ("hs", 2), ("down", 3), ("comb", 3), ("hr", 2), ("hr", 1), ("hr", 0),
            ("down", 2), ("comb", 2), ("down", 1), ("comb", 1), ("down", 0), ("comb", 0),
        ]
    late = list(range(2, groups)) + [g for g in (1, 0) if g < groups]
    steps = [("first",), ("gs", 0), ("gr", 0)]
    if groups > 1:
        steps += [("gs", 1)]
    steps += [("loaded",)]
    for g in range(groups):
        steps += [("ge", g), ("xs", g), ("up", g)]
        if g == 0 and groups > 1:
            steps += [("gr", 1)]
        if g + 2 < groups:
            steps += [("gs", g + 2)]
        if g and g + 1 < groups:
            steps += [("gr", g + 1)]
        if g == groups - 1 and g > 2:
            steps += [("hr", g - 1)]
        steps += [("hs", g)]
    relayed = [late[0]] if groups > 3 else []
    steps += [("down", g) for g in relayed]
    steps += [("hr", g) for g in late if g not in relayed]
    steps += [("comb", g) for g in relayed]
    for g in late:
        if g not in relayed:
            steps += [("down", g), ("comb", g)]
    return steps


def returned(steps, per):
    late = [of[0] for name, *of in steps if name == "comb"]
    return [k for g in late for k in range(g * per, (g + 1) * per) if k] + [0]


def kernel(
    n, planes, groups, wide,
    tokens_hbm, gain_hbm, routing_hbm, weight_hbm, gate_hbm, up_hbm, down_hbm, final_hbm,
    out,
    tokens, routing_t, weight_t, final_gain,
    wg, wu, wd, gains, picked, chosen_wide, x, xn, hid, half_own, half_send, half_recv, pair, comb, sq_out, sq_in,
    in_sem, w_sem, out_sem, gain_r, tok_r, disp_r, wide_r, x_r, d2d_r, h_r, po_r, c_r, sq_r,
):
    ep, t = lax.axis_index("ep"), lax.axis_index("tp")
    z, core = ep // 2, ep % 2
    partner = (ep + 1 - 2 * core, t)
    pieces, cap, part = picked.shape[1:]
    width = pieces * part
    per = planes // groups
    rows = per * cap
    inner = hid.shape[-1]
    tok_rows = tokens.shape[1]
    depth = n * width
    tp_peer = [(ep, flipped(t, j)) for j in range(n)]
    tp_index = [flipped(t, j) for j in range(n)]
    expert = [flipped(z, k) for k in range(planes)]
    plane_peer = [(2 * expert[k] + core, t) for k in range(planes)]
    narrow = [k for k in range(1, planes) if k // per not in wide]
    gathered = [g for g in range(groups) if not wide or (g and g not in wide)]

    barrier = pltpu.get_barrier_semaphore()
    peers = tp_peer[1:] + plane_peer[1:] + [partner]
    for peer in peers:
        pl.semaphore_signal(barrier, inc=1, device_id=peer, device_id_type=MESH)

    inputs = [
        pltpu.make_async_copy(src, dst, in_sem.at[i])
        for i, (src, dst) in enumerate((
            (tokens_hbm, tokens.at[0]), (routing_hbm, routing_t), (gain_hbm, gains.at[0]),
            (weight_hbm, weight_t), (final_hbm, final_gain),
        ))
    ]
    loads = [
        pltpu.make_async_copy(src.at[0], dst, w_sem.at[i])
        for i, (src, dst) in enumerate(((gate_hbm, wg), (up_hbm, wu), (down_hbm, wd)))
    ]
    for load in inputs + loads:
        load.start()
    for load in inputs[:3]:
        load.wait()

    token_row = lax.broadcasted_iota(jnp.int32, (tok_rows, tok_rows), 0)
    token_col = lax.broadcasted_iota(jnp.int32, (tok_rows, tok_rows), 1)
    r_t0, r_t1 = routing_t[0:1, :], routing_t[1:2, :]
    tall = -(-planes // 16) * 16
    sub = lax.broadcasted_iota(jnp.int32, (tall, tok_rows), 0)
    member_t = jnp.zeros((tall, tok_rows), F32)
    for k in range(planes):
        named = ((r_t0 == expert[k]) | (r_t1 == expert[k])).astype(F32)
        member_t = jnp.where(sub == k, named, member_t)
    earlier = (token_row < token_col).astype(F32).astype(BF16)
    slot_t = dot(member_t.astype(BF16), earlier)
    slot_t = jnp.where(member_t > 0, slot_t, -1.0)
    slot_sub = lax.broadcasted_iota(jnp.int32, (cap, tok_rows), 0).astype(F32)

    def pick(k, j, to):
        chosen = (slot_sub == slot_t[k : k + 1, :]).astype(F32).astype(BF16)
        found = dot(chosen, tokens[j]).astype(BF16)
        for i in range(pieces):
            to[i] = found[:, i * part : (i + 1) * part]

    def remote(src, dst, s, r, peer):
        return pltpu.make_async_remote_copy(
            src_ref=src, dst_ref=dst, send_sem=s, recv_sem=r, device_id=peer, device_id_type=MESH
        )

    sent = {}

    def start(copy, sem, ref):
        copy.start()
        sent[sem] = ref
        return copy

    class Cast:
        def __init__(self, at, whole, ways, sem, total, slot):
            self.at, self.whole, self.sem, self.total, self.slot = at, whole, sem, total, slot
            self.trees = [spread(n, backwards) for backwards in ways]
            self.slots = arrivals(n, ways)[0]
            self.copies = [
                {
                    into: remote(at(i, j), at(i, into), out_sem.at[sem], slot(self.slots[i, into]), tp_peer[bit])
                    for j, into, bit in edges
                }
                for i, (edges, _, _) in enumerate(self.trees)
            ]

        def begin(self):
            for step in range(n.bit_length() - 1):
                for i, (_, need, _) in enumerate(self.trees):
                    start(self.copies[i][need[0][step]], self.sem, self.total)

        def relay(self, then=None):
            for i, (_, need, come) in enumerate(self.trees):
                for j in come:
                    if need[j]:
                        self.copies[i][j].wait_recv()
                        for into in need[j]:
                            start(self.copies[i][into], self.sem, self.total)
                        if then:
                            then(i, j)

        def settle(self, j, then=None, then_all=None):
            ends = [i for i, (_, need, _) in enumerate(self.trees) if not need[j]]
            if len(ends) == len(self.trees):
                ref = self.whole(j)
                remote(ref, ref, out_sem.at[self.sem], self.slot(self.slots[0, j]), tp_peer[j]).wait_recv()
                if then_all:
                    then_all(j)
                return
            for i in ends:
                self.copies[i][j].wait_recv()
                if then:
                    then(i, j)

    TOK, DISP, WIDE, X, D2D, H, PO, C, SQ, GAIN = range(10)

    with scope("picks"):
        pick(0, 0, x.at[0, 0, 0, :, 0])
        for at, k in enumerate(narrow):
            pick(k, 0, picked.at[at])
        for at, k in enumerate(wide):
            pick(k, 0, chosen_wide.at[at, 0])

    with scope("barrier"):
        pl.semaphore_wait(barrier, len(peers))

    disp = {
        k: remote(
            picked.at[at], x.at[k // per, 0, 0, :, k % per], out_sem.at[DISP], disp_r.at[at], plane_peer[k]
        )
        for at, k in enumerate(narrow)
    }

    def across(g, j):
        start(
            remote(x.at[g, j, 0], x.at[g, j, 1], out_sem.at[D2D], d2d_r.at[g], partner), D2D, x.at[:, :, 0]
        )

    def across_piece(g):
        return lambda i, j: start(
            remote(x.at[g, j, 0, i], x.at[g, j, 1, i], out_sem.at[D2D], d2d_r.at[g], partner), D2D, x.at[:, :, 0]
        )

    def across_end(g):
        ref = x.at[g, :, 1]
        remote(ref, ref, out_sem.at[D2D], d2d_r.at[g], partner).wait_recv()

    def wide_copy(at, j):
        k = wide[at]
        return remote(
            chosen_wide.at[at, j], x.at[k, j, 0, :, 0], out_sem.at[WIDE], wide_r.at[at, j], plane_peer[k]
        )

    if wide:
        quarters = len(ways_of_tokens(tok_rows))
        tall_piece = tok_rows // quarters
        token_cast = Cast(
            lambda i, j: tokens.at[j, i * tall_piece : (i + 1) * tall_piece], lambda j: tokens.at[j],
            ways_of_tokens(tok_rows), TOK, tokens.at[0 : n - 1], lambda slot: tok_r.at[slot],
        )
    x_casts = {
        g: Cast(
            lambda i, j, g=g: x.at[g, j, 0, i], lambda j, g=g: x.at[g, j, 0],
            ways_of(pieces, g), X, x.at[gathered[0] :, 0 : n - 1, 0],
            lambda slot, at=at: x_r.at[at, slot],
        )
        for at, g in enumerate(gathered)
    }
    h_casts = [
        Cast(
            lambda i, j, g=g: hid.at[g, j, i], lambda j, g=g: hid.at[g, j],
            [False, True], H, hid.at[:, 0 : n - 1], lambda slot, g=g: h_r.at[g, slot],
        )
        for g in range(groups)
    ]
    gain_copies = [
        remote(gains.at[0], gains.at[j], out_sem.at[GAIN], gain_r.at[0], tp_peer[j]) for j in range(1, n)
    ]

    def first():
        if wide:
            token_cast.begin()
            across(0, 0)
        for copy in gain_copies:
            start(copy, GAIN, gains.at[1:])
        for k in narrow:
            start(disp[k], DISP, picked)
        for at in range(len(wide)):
            start(wide_copy(at, 0), WIDE, chosen_wide)

    def tokens_end():
        for j in range(1, n):
            token_cast.settle(j)
            pick(0, j, x.at[0, j, 0, :, 0])
            across(0, j)
            for at, k in enumerate(wide):
                pick(k, j, chosen_wide.at[at, j])
                start(wide_copy(at, j), WIDE, chosen_wide)

    def wide_end(g):
        for j in range(n):
            wide_copy(wide.index(g), j).wait_recv()
            across(g, j)

    def gather_start(g):
        for k in range(max(1, g * per), (g + 1) * per):
            disp[k].wait_recv()
        x_casts[g].begin()
        across(g, 0)

    def gather_end(g):
        for j in range(1, n):
            x_casts[g].settle(j, across_piece(g), lambda j: across(g, j))

    def loaded():
        remote(gains.at[1:], gains.at[1:], out_sem.at[GAIN], gain_r.at[0], partner).wait_recv()
        for load in inputs[3:] + loads:
            load.wait()

    def upward(g):
        blocks = [
            [x[g, j, :, i].reshape(2 * rows, part).astype(F32) for i in range(pieces)] for j in range(n)
        ]
        square = sum(jnp.sum(p * p, axis=1, keepdims=True) for of_peer in blocks for p in of_peer)
        scale = lax.rsqrt(square / depth + EPS)
        for j in range(n):
            for i in range(pieces):
                columns = pl.ds(pl.multiple_of(tp_index[j] * width + i * part, part), part)
                own = gains[j, :, i * part : (i + 1) * part]
                xn[:, columns] = (blocks[j][i] * scale * own).astype(BF16)
        for first in range(0, inner, 256):
            last = min(first + 256, inner)
            left = dot(xn[...], wg[:, first:last])
            right = dot(xn[...], wu[:, first:last])
            value = (jax.nn.silu(left) * right).astype(BF16)
            hid[g, 0, :, :, first:last] = value.reshape(2, rows, last - first)

    halves = [
        remote(half_send.at[g], half_recv.at[g], out_sem.at[PO], po_r.at[g], partner) for g in range(groups)
    ]

    def downward(g):
        total = None
        for j in range(n):
            if j:
                h_casts[g].settle(j)
            block = wd[pl.ds(pl.multiple_of(tp_index[j] * inner, inner), inner), :]
            term = dot(hid[g, j].reshape(2 * rows, inner), block)
            total = term if total is None else total + term
        half_own[g] = total[:rows].astype(BF16)
        half_send[g] = total[rows:].astype(BF16)
        start(halves[g], PO, half_send)

    back = {
        k: remote(pair.at[k // per, k % per], comb.at[k], out_sem.at[C], c_r.at[k - 1], plane_peer[k])
        for k in range(1, planes)
    }

    def combine(g):
        halves[g].wait_recv()
        both = (half_own[g].astype(F32) + half_recv[g].astype(F32)).astype(BF16)
        pair[g] = both.reshape(per, cap, width)
        for k in range(g * per, (g + 1) * per):
            if k == 0:
                comb[0] = both[:cap]
            else:
                start(back[k], C, comb.at[1:])

    actions = dict(
        first=first, tend=tokens_end, gs=gather_start, ge=gather_end, xs=across_end, xw=wide_end, up=upward,
        loaded=loaded, hs=lambda g: h_casts[g].begin(), hr=lambda g: h_casts[g].relay(), down=downward,
        comb=combine, gr=lambda g: x_casts[g].relay(across_piece(g)), trelay=lambda: token_cast.relay(),
    )
    steps = order(groups, per, wide)
    for name, *of in steps:
        with scope(name + "".join(str(g) for g in of)):
            actions[name](*of)

    w_t0, w_t1 = weight_t[0:1, :], weight_t[1:2, :]

    def share(k):
        weight = jnp.where(r_t0 == expert[k], w_t0, w_t1)
        table = jnp.where(slot_sub == slot_t[k : k + 1, :], weight, 0.0)
        high = table.astype(BF16)
        rest = table - high.astype(F32)
        middle = rest.astype(BF16)
        low = (rest - middle.astype(F32)).astype(BF16)
        block = comb[k]
        return dot_t(high, block) + (dot_t(middle, block) + dot_t(low, block))

    mixed = None
    for k in returned(steps, per):
        with scope(f"share{k}"):
            if k:
                back[k].wait_recv()
            mixed = share(k) if mixed is None else mixed + share(k)

    square = jnp.sum(mixed * mixed, axis=1, keepdims=True)
    sq_out[...] = jnp.transpose(jnp.broadcast_to(square, (tok_rows, 128)))[0:8, :]
    for j in range(1, n):
        start(remote(sq_out, sq_in.at[j], out_sem.at[SQ], sq_r.at[0], tp_peer[j]), SQ, sq_in.at[1:])
    with scope("sqwait"):
        remote(sq_in.at[1:], sq_in.at[1:], out_sem.at[SQ], sq_r.at[0], partner).wait_recv()
    total = sq_out[...]
    for j in range(1, n):
        total = total + sq_in[j]
    column = jnp.transpose(jnp.broadcast_to(total[0:1, :], (128, tok_rows)))[:, 0:1]
    out[...] = (mixed * lax.rsqrt(column / depth + EPS) * final_gain[...]).astype(BF16)
    with scope("wsend"):
        for sem, ref in sent.items():
            remote(ref, ref, out_sem.at[sem], sq_r.at[0], partner).wait_send()


def ways_of_tokens(tok_rows):
    return [False, True] * (2 if tok_rows % 64 == 0 else 1)


def shards(
    tokens, norm_gain, routing, route_weight, gate_weight, up_weight, down_weight, final_gain
):
    ep_count, n = lax.axis_size("ep"), lax.axis_size("tp")
    planes = ep_count // 2
    tok_rows, width = tokens.shape
    capacity = 2 * ((tok_rows * TOPK * 5 + planes * 8 - 1) // (planes * 8))
    cap = -(-capacity // 16) * 16
    groups = min(4, planes)
    per = planes // groups
    rows = per * cap
    wide = wide_groups(planes, per)
    pieces = 2 if width % 256 == 0 else 1
    part = width // pieces
    depth, inner = gate_weight.shape[1:]
    few = max(1, len(wide))
    gathered = groups - 1 - len(wide) if wide else groups
    narrow = planes - 1 - len(wide)
    dma = pltpu.SemaphoreType.DMA
    vmem, anywhere = pl.BlockSpec(memory_space=pltpu.VMEM), pl.BlockSpec(memory_space=pl.ANY)
    return pl.pallas_call(
        functools.partial(kernel, n, planes, groups, wide),
        out_shape=pltpu.VMEM((tok_rows, width), BF16),
        in_specs=[anywhere] * 8,
        out_specs=vmem,
        scratch_shapes=[
            pltpu.VMEM((n if wide else 1, tok_rows, width), BF16),
            pltpu.VMEM((TOPK, tok_rows), jnp.int32),
            pltpu.VMEM((TOPK, tok_rows), F32),
            pltpu.VMEM((1, width), F32),
            pltpu.VMEM((depth, inner), BF16),
            pltpu.VMEM((depth, inner), BF16),
            pltpu.VMEM((n * inner, width), BF16),
            pltpu.VMEM((n, 1, width), F32),
            pltpu.VMEM((max(1, narrow), pieces, cap, part), BF16),
            pltpu.VMEM((few, n if wide else 1, pieces, cap, part), BF16),
            pltpu.VMEM((groups, n, 2, pieces, per, cap, part), BF16),
            pltpu.VMEM((2 * rows, depth), BF16),
            pltpu.VMEM((groups, n, 2, rows, inner), BF16),
            pltpu.VMEM((groups, rows, width), BF16),
            pltpu.VMEM((groups, rows, width), BF16),
            pltpu.VMEM((groups, rows, width), BF16),
            pltpu.VMEM((groups, per, cap, width), BF16),
            pltpu.VMEM((planes, cap, width), BF16),
            pltpu.VMEM((8, 128), F32),
            pltpu.VMEM((n, 8, 128), F32),
            dma((5,)), dma((3,)), dma((10,)), dma((1,)),
            dma((arrivals(n, ways_of_tokens(tok_rows))[1] if wide else 1,)),
            dma((max(1, narrow),)), dma((few, n if wide else 1)),
            dma((gathered, arrivals(n, ways_of(pieces, 0))[1])), dma((groups,)),
            dma((groups, arrivals(n, [False, True])[1])), dma((groups,)), dma((max(1, planes - 1),)), dma((1,)),
        ],
        compiler_params=pltpu.CompilerParams(
            collective_id=0, has_side_effects=True, vmem_limit_bytes=60 * 1024 * 1024
        ),
    )(
        tokens, norm_gain.reshape(1, width), routing.T, route_weight.T,
        gate_weight, up_weight, down_weight, final_gain.reshape(1, width),
    )


def solution(mesh):
    placed = (
        P("ep", "tp"),
        P("tp"),
        P("ep", None),
        P("ep", None),
        P("ep", None, "tp"),
        P("ep", None, "tp"),
        P("ep", None, "tp"),
        P("tp"),
    )
    return jax.shard_map(
        shards, mesh=mesh, in_specs=placed, out_specs=P("ep", "tp"), check_vma=False
    )
```
